32 devices in a mesh: fs: 16 (over z, y, x), tp: 2 (over core).
Axes of the slice: x: 2, y: 2, z: 4, core: 2. Of those that a mesh axis runs over, the one named last changes fastest.
Arguments:
- tokens: bfloat16 [12288, 2048], P('fs'), may hold values from -6 to 6
- norm_gain: float32 [2048], replicated, may hold values from 0.1 to 1.9
- gate_weight: float32 [2048, 5632], P('fs', 'tp'), may hold values from -0.125 to 0.125
- up_weight: float32 [2048, 5632], P('fs', 'tp'), may hold values from -0.125 to 0.125
- gate_scale: float32 [5632], P('tp'), may hold values from 0.1 to 1.9
- up_scale: float32 [5632], P('tp'), may hold values from 0.1 to 1.9
- down_weight: float32 [5632, 2048], P('tp', 'fs'), may hold values from -0.078125 to 0.078125
- down_scale: float32 [2048], P('tp'), may hold values from 0.1 to 1.9
Outputs:
- mixed: bfloat16 [12288, 2048], P('fs', 'tp')
The draws below stay inside these ranges and needn't reach their ends.
All inputs are finite; a program needn't handle non-finite values.
Results may differ from the reference program's by a relative error of at most 0.014.
Values may be sent and summed in bfloat16 or wider, within the bound.
A program may use at most 128 MiB of HBM per device.

```python
import jax
import jax.numpy as jnp
from jax import lax

D = 2048
FF = 5632
TOK_DEV = 768
TOKENS = 12288
N_FS = 16
N_TP = 2


def level_of(key, shape, cuts, low, high):
    loudness, own = 1.0, jax.random.fold_in(key, 6)
    for position, shards_of in cuts:
        draws = jnp.exp(jax.random.uniform(jax.random.fold_in(own, position), (shards_of,), jnp.float32, low / len(cuts), high / len(cuts)))
        loudness = loudness * jnp.repeat(draws, shape[position] // shards_of).reshape([-1 if axis == position else 1 for axis in range(len(shape))])
    return loudness


def centred(own_key, dims, spread, most, split=(), held_as=jnp.bfloat16):
    drawn = spread * jax.random.normal(own_key, dims, jnp.float32)
    if split:
        drawn = drawn * level_of(own_key, dims, split, -0.22, 0.18)
    return jnp.clip(drawn, -most, most).astype(held_as)


def setup_inputs(seed: int = 0) -> dict:
    arg_keys = jax.random.split(jax.random.key(seed), 9)
    return {
        "tokens": centred(arg_keys[0], (TOKENS, D), 1.0, 6.0, ((0, 16),)),
        "norm_gain": jnp.clip(1.0 + 0.18 * jax.random.normal(arg_keys[1], (D,), jnp.float32), 0.1, 1.9),
        "gate_weight": centred(arg_keys[2], (D, FF), D ** -0.5, 0.125, ((0, 16), (1, 2)), jnp.float32),
        "up_weight": centred(arg_keys[3], (D, FF), D ** -0.5, 0.125, ((0, 16), (1, 2)), jnp.float32),
        "gate_scale": jnp.clip(1.0 + 0.18 * jax.random.normal(arg_keys[4], (FF,), jnp.float32), 0.1, 1.9),
        "up_scale": jnp.clip(1.0 + 0.18 * jax.random.normal(arg_keys[5], (FF,), jnp.float32), 0.1, 1.9),
        "down_weight": centred(arg_keys[6], (FF, D), FF ** -0.5, 0.078125, ((0, 2), (1, 16)), jnp.float32),
        "down_scale": jnp.clip(1.0 + 0.18 * jax.random.normal(arg_keys[7], (D,), jnp.float32), 0.1, 1.9),
    }


def reference(tokens, norm_gain, gate_weight, up_weight, gate_scale, up_scale, down_weight, down_scale):
    gate_low = gate_weight.astype(jnp.bfloat16)
    up_low = up_weight.astype(jnp.bfloat16)
    down_low = down_weight.astype(jnp.bfloat16).reshape(N_TP, FF // N_TP, D)

    def one_block(rows):
        values = rows.astype(jnp.float32)
        normed = (values * lax.rsqrt(lax.optimization_barrier(jnp.mean(values * values, axis=-1, keepdims=True)) + 1e-06) * norm_gain).astype(jnp.bfloat16)
        gate = jnp.dot(normed, gate_low, preferred_element_type=jnp.float32) * gate_scale
        up = jnp.dot(normed, up_low, preferred_element_type=jnp.float32) * up_scale
        hidden = (jax.nn.silu(gate) * up).astype(jnp.bfloat16).reshape(rows.shape[0], N_TP, FF // N_TP)
        total = jnp.zeros((rows.shape[0], D), jnp.float32)
        for block in range(N_TP):
            partial_sum = jnp.dot(hidden[:, block], down_low[block], preferred_element_type=jnp.float32).astype(jnp.bfloat16)
            partial_sum = lax.optimization_barrier(partial_sum)
            total = total + partial_sum.astype(jnp.float32)
        return (total * down_scale).astype(jnp.bfloat16)
    blocks = lax.map(one_block, tokens.reshape(N_FS, TOK_DEV, D))
    return blocks.reshape(TOKENS, D)
```

```python
import jax
import jax.numpy as jnp
from jax import lax
from jax.experimental import pallas as pl
from jax.experimental.pallas import tpu as pltpu
from jax.sharding import PartitionSpec as P

MESH = pl.DeviceIdType.MESH
NN = (((1,), (0,)), ((), ()))
TILE = 128


def norm(tokens, norm_gain):
    values = tokens.astype(jnp.float32)
    return (
        values * lax.rsqrt(jnp.mean(values * values, axis=-1, keepdims=True) + 1e-06) * norm_gain
    ).astype(jnp.bfloat16)


def gathered(tokens, norm_gain, gate_weight, up_weight, gate_scale, up_scale, down_weight, down_scale):
    normed = norm(tokens, norm_gain)

    def add_rows(piece):
        return jnp.dot(normed, piece, preferred_element_type=jnp.float32)

    gate = add_rows(lax.all_gather(gate_weight.astype(jnp.bfloat16), "fs", axis=0, tiled=True))
    up = add_rows(lax.all_gather(up_weight.astype(jnp.bfloat16), "fs", axis=0, tiled=True))
    hidden = (jax.nn.silu(gate * gate_scale) * (up * up_scale)).astype(jnp.bfloat16)
    terms = jnp.dot(
        hidden,
        lax.all_gather(down_weight.astype(jnp.bfloat16), "fs", axis=1, tiled=True),
        preferred_element_type=jnp.float32,
    )
    summed = lax.psum_scatter(
        terms.astype(jnp.bfloat16), "tp", scatter_dimension=1, tiled=True
    ).astype(jnp.float32)
    return (summed * down_scale).astype(jnp.bfloat16)


def kernel(
    g_ref, u_ref, d_ref, x_ref, ng_ref, gs_ref, us_ref, ds_ref, out_ref,
    xbuf, wgu, wd, gsend, dsend, accg, accu, hid, pbuf, rbuf, scl,
    l_sem, rsh_send, rsh_recv, x_send, x_recv, s_send, s_recv,
    z_send, z_recv, p_send, p_recv, r_send, r_recv,
):
    f, c = lax.axis_index("fs"), lax.axis_index("tp")
    z, q = lax.div(f, 4), lax.rem(f, 4)
    qk = [q, q + 1 - 2 * lax.rem(q, 2), lax.rem(q + 2, 4), 3 - q]
    tiles = gsend.shape[1]
    hi = wgu.shape[2]
    lo = tiles // 4
    rows = x_ref.shape[0]
    half, quarter = rows // 2, rows // 4
    width = 4 * TILE
    pair = 2 * TILE
    big = lax.rem(q + c, 2) == 0
    small = lax.rem(q + c, 2) != 0
    partner = (f, 1 - c)

    def at(k):
        return (4 * z + qk[k], c)

    def first(k):
        return lo * qk[k] + lax.div(qk[k] + 1 - c, 2)

    def chip(k):
        return lax.rem(q + k, 2) + 2 * lax.rem(lax.div(q, 2) + lax.div(k, 2), 2)

    def rcopy(src, dst, ssem, rsem, dev):
        return pltpu.make_async_remote_copy(
            src_ref=src, dst_ref=dst, send_sem=ssem, recv_sem=rsem,
            device_id=dev, device_id_type=MESH,
        )

    barrier = pltpu.get_barrier_semaphore()

    def greet(dev):
        pl.semaphore_signal(barrier, inc=1, device_id=dev, device_id_type=MESH)

    greet(partner)
    for k in (1, 2, 3):
        greet(at(k))
    pl.when(z > 0)(lambda: greet((f - 4, c)))
    pl.when(z < 3)(lambda: greet((f + 4, c)))

    slab = hi * TILE
    cuts = [(i, min(slab, tiles * TILE - i)) for i in range(0, tiles * TILE, slab)]
    loads = ([], [])
    for j, ref in enumerate((g_ref, u_ref)):
        for n, (i, w) in enumerate(cuts):
            loads[j].append(pltpu.make_async_copy(
                ref.at[:, pl.ds(i, w)],
                accg.at[pl.ds((j * len(cuts) + n) * TILE, TILE), pl.ds(0, w)],
                l_sem.at[j, n],
            ))
    load_d = pltpu.make_async_copy(
        d_ref, accu.at[pl.ds(0, tiles * TILE), pl.ds(0, TILE)], l_sem.at[2, 0]
    )
    mine = pl.ds(pl.multiple_of(half * c, 16), half)
    load_x = pltpu.make_async_copy(x_ref.at[mine, :], xbuf.at[q, mine, :], l_sem.at[2, 1])
    for j in (0, 1):
        for copy in loads[j]:
            copy.start()
    load_d.start()
    load_x.start()

    @pl.when(small)
    def _():
        nothing = jnp.zeros((TILE, TILE), jnp.bfloat16)

        def step(i, _):
            wgu[i, 0, hi - 1] = nothing
            wgu[i, 1, hi - 1] = nothing
            wd[i, hi - 1] = nothing
            return 0

        lax.fori_loop(0, 16, step, 0)

    start = first(0)
    for j, ref in enumerate((gs_ref, us_ref)):
        scl[j : j + 1, : lo * TILE] = ref[:, pl.ds(pl.multiple_of(start * TILE, TILE), lo * TILE)]
        last = jnp.minimum(start + lo, tiles - 1)
        scl[j : j + 1, lo * TILE :] = ref[:, pl.ds(pl.multiple_of(last * TILE, TILE), TILE)]

    for j in (0, 1):
        for copy in loads[j]:
            copy.wait()
        for i in range(tiles):
            n, m = divmod(i, hi)
            gsend[j, i] = accg[
                (j * len(cuts) + n) * TILE : (j * len(cuts) + n + 1) * TILE,
                m * TILE : (m + 1) * TILE,
            ].astype(jnp.bfloat16)
        for i in range(lo):
            wgu[f, j, i] = gsend[j, start + i]

    @pl.when(big)
    def _():
        for j in (0, 1):
            wgu[f, j, hi - 1] = gsend[j, start + hi - 1]

    slot = [wgu, wd]

    def cut(cls, i, n):
        return wgu.at[i, :, pl.ds(0, n)] if cls == 0 else wd.at[i, pl.ds(0, n)]

    def stored(cls, k, n):
        return gsend.at[:, pl.ds(first(k), n)] if cls == 0 else dsend.at[pl.ds(first(k), n)]

    def sized(fn):
        pl.when(big)(lambda: fn(hi))
        pl.when(small)(lambda: fn(lo))

    def swapped(fn):
        pl.when(small)(lambda: fn(hi))
        pl.when(big)(lambda: fn(lo))

    def rsh(cls, k, n):
        return rcopy(
            stored(cls, k, n), cut(cls, f, n),
            rsh_send.at[cls, k - 1], rsh_recv.at[cls, k - 1], at(k),
        )

    def rsh_arrived(cls, k, n):
        where = cut(cls, 4 * z + qk[k], n)
        return rcopy(where, where, rsh_send.at[cls, k - 1], rsh_recv.at[cls, k - 1], at(k))

    def rsh_start(cls, k):
        (sized if k == 2 else swapped)(lambda n: rsh(cls, k, n).start())

    def rsh_wait_send(cls, k):
        (sized if k == 2 else swapped)(lambda n: rsh(cls, k, n).wait_send())

    def rsh_wait(cls, k):
        sized(lambda n: rsh_arrived(cls, k, n).wait_recv())

    def zcopy(cls, i, d, n):
        dev = (f + 4, c) if d == 0 else (f - 4, c)
        return rcopy(cut(cls, i, n), cut(cls, i, n), z_send.at[d, cls, i], z_recv.at[cls, i], dev)

    def inward(cls, i):
        pl.when(z < 2)(lambda: sized(lambda n: zcopy(cls, i, 0, n).start()))
        pl.when(z > 1)(lambda: sized(lambda n: zcopy(cls, i, 1, n).start()))

    def outward(cls, i):
        pl.when(z == 2)(lambda: sized(lambda n: zcopy(cls, i, 0, n).start()))
        pl.when(z == 1)(lambda: sized(lambda n: zcopy(cls, i, 1, n).start()))

    def relay(cls, r, ks):
        for k in ks:
            low = 4 * (z - r) + qk[k]
            high = 4 * (z + r) + qk[k]

            @pl.when(z >= r)
            def _():
                sized(lambda n: zcopy(cls, low, 0, n).wait_recv())
                if r < 3:
                    pl.when(z < 3)(lambda: sized(lambda n: zcopy(cls, low, 0, n).start()))

            @pl.when(z + r <= 3)
            def _():
                sized(lambda n: zcopy(cls, high, 1, n).wait_recv())
                if r < 3:
                    pl.when(z > 0)(lambda: sized(lambda n: zcopy(cls, high, 1, n).start()))

    pl.semaphore_wait(barrier, 4 + jnp.minimum(z, 1) + jnp.minimum(3 - z, 1))
    outward(0, f)
    inward(0, f)
    for k in (1, 2, 3):
        rsh_start(0, k)

    load_d.wait()
    for i in range(tiles):
        dsend[i] = accu[i * TILE : (i + 1) * TILE, :TILE].astype(jnp.bfloat16)
    for i in range(lo):
        wd[f, i] = dsend[start + i]

    @pl.when(big)
    def _():
        wd[f, hi - 1] = dsend[start + hi - 1]

    load_x.wait()

    def normalize(m, _):
        here = pl.ds(pl.multiple_of(half * c + m * 16, 16), 16)
        values = xbuf[q, here, :].astype(jnp.float32)
        scale = lax.rsqrt(jnp.mean(values * values, axis=-1, keepdims=True) + 1e-06)
        xbuf[q, here, :] = (values * scale * ng_ref[...]).astype(jnp.bfloat16)
        return 0

    lax.fori_loop(0, half // 16, normalize, 0)

    def piece(core, h):
        return pl.ds(pl.multiple_of(half * core + h * quarter, 16), quarter)

    def xcopy(owner, h, ssem, rsem, dev):
        where = xbuf.at[qk[owner], piece(c, h), :]
        return rcopy(where, where, ssem, rsem, dev)

    def direct(k, h, owner):
        return xcopy(owner, h, x_send.at[k - 1, h], x_recv.at[k - 1, h], at(k))

    def onward(h, owner):
        return xcopy(owner, h, x_send.at[2, h], x_recv.at[2, h], at(2 if h == 0 else 1))

    def share(k, h, core):
        where = xbuf.at[qk[k], piece(core, h), :]
        return rcopy(where, where, s_send.at[k, h], s_recv.at[k, h], partner)

    outward(1, f)
    inward(1, f)
    for k in (1, 2, 3):
        rsh_start(1, k)
    direct(1, 0, 0).start()
    direct(2, 1, 0).start()
    direct(1, 1, 0).start()
    direct(2, 0, 0).start()
    for h in (0, 1):
        share(0, h, c).start()

    for k in (1, 2, 3):
        rsh_wait(0, k)
        outward(0, 4 * z + qk[k])
        inward(0, 4 * z + qk[k])

    side = lax.div(z, 2)
    zz = z + side * (3 - 2 * z)

    def turn(t):
        base = t if t >= 2 else lax.rem(t + zz, 2)
        return base + side * (3 - 2 * base)

    def columns(s, h=None):
        if h is None:
            return pl.ds(pl.multiple_of(s * width, TILE), width)
        return pl.ds(pl.multiple_of(s * width + h * pair, TILE), pair)

    def gate_up(t, k0, k1):
        s = turn(t)

        def step(m, _):
            who = chip(lax.div(m, hi // 2))
            n = lax.rem(m, hi // 2)
            here = pl.ds(pl.multiple_of(who * rows, 16), rows)
            cols = pl.ds(pl.multiple_of(n * pair, TILE), pair)
            found = []
            for j, acc in enumerate((accg, accu)):
                w = jnp.concatenate([
                    jnp.concatenate([wgu[4 * s + i, j, 2 * n], wgu[4 * s + i, j, 2 * n + 1]], axis=1)
                    for i in range(4)
                ], axis=0)
                x = xbuf[who, :, columns(s)]
                part_sum = lax.dot_general(x, w, NN, preferred_element_type=jnp.float32)
                if t > 0:
                    part_sum = part_sum + acc[here, cols]
                if t < 3:
                    acc[here, cols] = part_sum
                found.append(part_sum)
            if t == 3:
                g = found[0] * scl[0:1, cols]
                u = found[1] * scl[1:2, cols]
                hid[here, cols] = (g / (1.0 + jnp.exp(-g)) * u).astype(jnp.bfloat16)
            return 0

        lax.fori_loop(k0 * (hi // 2), k1 * (hi // 2), step, 0)

    relay(0, 1, range(4))
    for h in (0, 1):
        share(0, h, 1 - c).wait_recv()
    direct(1, 0, 1).wait_recv()
    onward(0, 1).start()
    share(1, 0, c).start()
    direct(2, 1, 2).wait_recv()
    onward(1, 2).start()
    share(2, 1, c).start()
    for k in (1, 2, 3):
        rsh_wait(1, k)
        inward(1, 4 * z + qk[k])
    relay(0, 2, range(3))
    direct(1, 1, 1).wait_recv()
    share(1, 1, c).start()
    direct(2, 0, 2).wait_recv()
    share(2, 0, c).start()
    for k in (1, 2):
        for h in (0, 1):
            share(k, h, 1 - c).wait_recv()
    gate_up(0, 0, 3)
    relay(0, 2, range(3, 4))
    for k in (1, 2, 3):
        outward(1, 4 * z + qk[k])
    gate_up(1, 0, 3)
    gate_up(2, 0, 3)
    onward(0, 3).wait_recv()
    share(3, 0, c).start()
    onward(1, 3).wait_recv()
    share(3, 1, c).start()
    for h in (0, 1):
        share(3, h, 1 - c).wait_recv()
    gate_up(0, 3, 4)
    gate_up(1, 3, 4)
    gate_up(2, 3, 4)
    for h in (0, 1):
        direct(1, h, 0).wait_send()
        direct(2, h, 0).wait_send()
        onward(h, 1 + h).wait_send()
        for k in range(4):
            share(k, h, c).wait_send()
    relay(0, 3, range(4))
    gate_up(3, 0, 4)

    order = (3, 1, 2, 0)

    def pcopy(s, k):
        i = lax.rem(s, 2)
        return rcopy(
            xbuf.at[qk[k], :, columns(s)], pbuf.at[i, k],
            p_send.at[i, k], p_recv.at[i, k], partner,
        )

    places = ((1, 0, 1), (3, 0, 1), (2, 1, 2), (3, 1, 2), (2, 0, 2), (1, 1, 1))

    def scopy(s, place):
        i = lax.rem(s, 2)
        k, h, to = places[place]
        return rcopy(
            xbuf.at[qk[k], :, columns(s, h)], rbuf.at[i, place],
            r_send.at[i, place], r_recv.at[i, place], at(to),
        )

    def added(where, cols, more):
        def step(m, _):
            here = pl.ds(pl.multiple_of(m * TILE, 16), TILE)
            both = xbuf[where, here, cols].astype(jnp.float32) + more[here, :].astype(jnp.float32)
            xbuf[where, here, cols] = both.astype(jnp.bfloat16)
            return 0

        lax.fori_loop(0, rows // TILE, step, 0)

    def finish(s, k):
        @pl.when(lax.div(s, 2) == c)
        def _():
            pcopy(s, k).wait_recv()
            added(qk[k], columns(s), pbuf.at[lax.rem(s, 2), k])
            for place in range(4):
                if places[place][0] == k:
                    scopy(s, place).start()

    def down(t):
        s = turn(t)
        for n, k in enumerate(order):
            here = pl.ds(pl.multiple_of(qk[k] * rows, 16), rows)

            def step(h, _):
                w = jnp.concatenate(
                    [wd[4 * s + 2 * h + i].reshape(hi * TILE, TILE) for i in (0, 1)], axis=1
                )
                o = lax.dot_general(hid[here, :], w, NN, preferred_element_type=jnp.float32)
                xbuf[qk[k], :, columns(s, h)] = o.astype(jnp.bfloat16)
                return 0

            lax.fori_loop(0, 2, step, 0)
            pl.when(lax.div(s, 2) != c)(lambda: pcopy(s, k).start())
            if n:
                finish(s, order[n - 1])
        finish(s, order[-1])

    def second(t):
        s = turn(t)

        @pl.when(lax.div(s, 2) == c)
        def _():
            i = lax.rem(s, 2)
            for came, goes in ((1, 4), (3, 5)):
                scopy(s, came).wait_recv()
                k, h, _ = places[goes]
                added(qk[k], columns(s, h), rbuf.at[i, came])
                scopy(s, goes).start()

    def result(i, h):
        s = 2 * c + i
        cols = pl.ds(pl.multiple_of(i * width + h * pair, TILE), pair)
        return pltpu.make_async_copy(xbuf.at[q, :, columns(s, h)], out_ref.at[:, cols], l_sem.at[i, h])

    def final(t):
        s = turn(t)

        @pl.when(lax.div(s, 2) == c)
        def _():
            i = lax.rem(s, 2)
            for h, (one, two) in enumerate(((0, 4), (2, 5))):
                scopy(s, one).wait_recv()
                scopy(s, two).wait_recv()
                cols = pl.ds(pl.multiple_of(i * width + h * pair, TILE), pair)

                def step(m, _):
                    here = pl.ds(pl.multiple_of(m * TILE, 16), TILE)
                    total = (
                        xbuf[q, here, columns(s, h)].astype(jnp.float32)
                        + rbuf[i, one, here, :].astype(jnp.float32)
                        + rbuf[i, two, here, :].astype(jnp.float32)
                    )
                    xbuf[q, here, columns(s, h)] = (total * ds_ref[:, cols]).astype(jnp.bfloat16)
                    return 0

                lax.fori_loop(0, rows // TILE, step, 0)
                result(i, h).start()

    down(0)
    relay(1, 1, range(4))
    down(1)
    second(0)
    relay(1, 2, range(4))
    down(2)
    second(1)
    second(2)
    relay(1, 3, range(4))
    down(3)
    final(0)
    final(1)
    final(2)
    second(3)
    final(3)

    for cls in (0, 1):
        for k in (1, 2, 3):
            rsh_wait_send(cls, k)
        for r in range(3):
            for k in range(4):
                low, high = 4 * (z - r) + qk[k], 4 * (z + r) + qk[k]
                pl.when((z >= r) & (z < 3))(
                    lambda: sized(lambda n: zcopy(cls, low, 0, n).wait_send())
                )
                pl.when((z + r <= 3) & (z > 0))(
                    lambda: sized(lambda n: zcopy(cls, high, 1, n).wait_send())
                )
    for i in range(2):
        for h in (0, 1):
            result(i, h).wait()
        for k in range(4):
            pcopy(2 * (1 - c) + i, k).wait_send()
        for place in range(6):
            scopy(2 * c + i, place).wait_send()


def planes(tokens, norm_gain, gate_weight, up_weight, gate_scale, up_scale, down_weight, down_scale):
    rows, model = tokens.shape
    units = gate_weight.shape[1]
    tiles = units // TILE
    hi = -(-tiles // 4)
    bf, f32, dma = jnp.bfloat16, jnp.float32, pltpu.SemaphoreType.DMA
    hbm = pl.BlockSpec(memory_space=pl.ANY)
    vmem = pl.BlockSpec(memory_space=pltpu.VMEM)
    return pl.pallas_call(
        kernel,
        out_shape=jax.ShapeDtypeStruct((rows, down_scale.shape[0]), bf),
        in_specs=[hbm, hbm, hbm, hbm, vmem, vmem, vmem, vmem],
        out_specs=hbm,
        scratch_shapes=[
            pltpu.VMEM((4, rows, model), bf),
            pltpu.VMEM((16, 2, hi, TILE, TILE), bf),
            pltpu.VMEM((16, hi, TILE, TILE), bf),
            pltpu.VMEM((2, tiles, TILE, TILE), bf),
            pltpu.VMEM((tiles, TILE, TILE), bf),
            pltpu.VMEM((4 * rows, hi * TILE), f32),
            pltpu.VMEM((4 * rows, hi * TILE), f32),
            pltpu.VMEM((4 * rows, hi * TILE), bf),
            pltpu.VMEM((2, 4, rows, 4 * TILE), bf),
            pltpu.VMEM((2, 6, rows, 2 * TILE), bf),
            pltpu.VMEM((8, hi * TILE), f32),
            dma((3, 4)), dma((2, 3)), dma((2, 3)),
            dma((3, 2)), dma((3, 2)), dma((4, 2)), dma((4, 2)),
            dma((2, 2, 16)), dma((2, 16)),
            dma((2, 4)), dma((2, 4)), dma((2, 6)), dma((2, 6)),
        ],
        compiler_params=pltpu.CompilerParams(
            collective_id=0, has_side_effects=True, vmem_limit_bytes=67043328
        ),
    )(
        gate_weight, up_weight, down_weight, tokens,
        norm_gain[None], gate_scale[None], up_scale[None], down_scale[None],
    )


def solution(mesh):
    in_specs = (
        P("fs", None),
        P(),
        P("fs", "tp"),
        P("fs", "tp"),
        P("tp"),
        P("tp"),
        P("tp", "fs"),
        P("tp"),
    )
    out_specs = P("fs", "tp")
    body = planes if (mesh.shape["fs"], mesh.shape["tp"]) == (16, 2) else gathered
    return jax.shard_map(body, mesh=mesh, in_specs=in_specs, out_specs=out_specs, check_vma=False)
```

```python
import jax
import jax.numpy as jnp
from jax import lax
from jax.experimental import pallas as pl
from jax.experimental.pallas import tpu as pltpu
from jax.sharding import PartitionSpec as P

MESH = pl.DeviceIdType.MESH
NN = (((1,), (0,)), ((), ()))
TILE = 128


def norm(tokens, norm_gain):
    values = tokens.astype(jnp.float32)
    return (
        values * lax.rsqrt(jnp.mean(values * values, axis=-1, keepdims=True) + 1e-06) * norm_gain
    ).astype(jnp.bfloat16)


def gathered(tokens, norm_gain, gate_weight, up_weight, gate_scale, up_scale, down_weight, down_scale):
    normed = norm(tokens, norm_gain)

    def add_rows(piece):
        return jnp.dot(normed, piece, preferred_element_type=jnp.float32)

    gate = add_rows(lax.all_gather(gate_weight.astype(jnp.bfloat16), "fs", axis=0, tiled=True))
    up = add_rows(lax.all_gather(up_weight.astype(jnp.bfloat16), "fs", axis=0, tiled=True))
    hidden = (jax.nn.silu(gate * gate_scale) * (up * up_scale)).astype(jnp.bfloat16)
    terms = jnp.dot(
        hidden,
        lax.all_gather(down_weight.astype(jnp.bfloat16), "fs", axis=1, tiled=True),
        preferred_element_type=jnp.float32,
    )
    summed = lax.psum_scatter(
        terms.astype(jnp.bfloat16), "tp", scatter_dimension=1, tiled=True
    ).astype(jnp.float32)
    return (summed * down_scale).astype(jnp.bfloat16)


def kernel(
    g_ref, u_ref, d_ref, x_ref, ng_ref, gs_ref, us_ref, ds_ref, out_ref,
    xbuf, wg, wu, wd, gsend, usend, dsend, accg, accu, hid, pbuf, rbuf, scl,
    l_sem, rsh_send, rsh_recv, x_send, x_recv, s_send, s_recv,
    z_send, z_recv, p_send, p_recv, r_send, r_recv,
):
    f, c = lax.axis_index("fs"), lax.axis_index("tp")
    z, q = lax.div(f, 4), lax.rem(f, 4)
    qk = [q, q + 1 - 2 * lax.rem(q, 2), lax.rem(q + 2, 4), 3 - q]
    slot, sends = (wg, wu, wd), (gsend, usend, dsend)
    part = wd.shape[1]
    tiles, full, odd = 4 * part // TILE, part // TILE, part % TILE
    hi = full + 1
    rows = x_ref.shape[0]
    half, quarter = rows // 2, rows // 4
    width = 4 * TILE
    pair = 2 * TILE
    partner = (f, 1 - c)

    def at(k):
        return (4 * z + qk[k], c)

    def chip(k):
        return lax.rem(q + k, 2) + 2 * lax.rem(lax.div(q, 2) + lax.div(k, 2), 2)

    def rcopy(src, dst, ssem, rsem, dev):
        return pltpu.make_async_remote_copy(
            src_ref=src, dst_ref=dst, send_sem=ssem, recv_sem=rsem,
            device_id=dev, device_id_type=MESH,
        )

    barrier = pltpu.get_barrier_semaphore()

    def greet(dev):
        pl.semaphore_signal(barrier, inc=1, device_id=dev, device_id_type=MESH)

    greet(partner)
    for k in (1, 2, 3):
        greet(at(k))
    pl.when(z > 0)(lambda: greet((f - 4, c)))
    pl.when(z < 3)(lambda: greet((f + 4, c)))

    slab = hi * TILE
    cuts = [(i, min(slab, tiles * TILE - i)) for i in range(0, tiles * TILE, slab)]
    loads = ([], [])
    for j, ref in enumerate((g_ref, u_ref)):
        for n, (i, w) in enumerate(cuts):
            loads[j].append(pltpu.make_async_copy(
                ref.at[:, pl.ds(i, w)],
                accg.at[pl.ds((j * len(cuts) + n) * TILE, TILE), pl.ds(0, w)],
                l_sem.at[j, n],
            ))
    load_d = pltpu.make_async_copy(
        d_ref, accu.at[pl.ds(0, tiles * TILE), pl.ds(0, TILE)], l_sem.at[2, 0]
    )
    mine = pl.ds(pl.multiple_of(half * c, 16), half)
    load_x = pltpu.make_async_copy(x_ref.at[mine, :], xbuf.at[q, mine, :], l_sem.at[2, 1])
    for copy in loads[0]:
        copy.start()

    def turned(value):
        return pltpu.roll(value, odd, 1)

    left = lax.broadcasted_iota(jnp.int32, (odd, TILE), 1) < odd
    whole = [full * n + (n + 1) // 2 for n in range(4)]
    split = [full + (full + hi) * (n // 2) for n in range(4)]
    for j, ref in enumerate((gs_ref, us_ref)):
        row = jnp.broadcast_to(ref[pl.ds(full + (full + hi) * lax.div(q, 2), 1), :], (8, TILE))
        row = jnp.where(lax.rem(q, 2) == 0, row, turned(row))
        scl[j : j + 1, :TILE] = row[0:1]
        for i in range(full):
            at_tile = full * q + lax.div(q + 1, 2) + i
            scl[j : j + 1, (i + 1) * TILE : (i + 2) * TILE] = ref[pl.ds(at_tile, 1), :]

    for copy in loads[1]:
        copy.start()
    load_d.start()
    load_x.start()

    def rounded(cls):
        def tile(i):
            if cls == 2:
                return accu[i * TILE : (i + 1) * TILE, :TILE]
            top = (cls * len(cuts) + i // hi) * TILE
            return accg[top : top + TILE, i % hi * TILE : (i % hi + 1) * TILE]

        for n in range(4):
            both = tile(split[n])
            top, low = both[:odd], both[odd:]
            if cls == 2:
                half_tile = top if n % 2 == 0 else low
            elif n % 2 == 0:
                half_tile = jnp.where(left, top, turned(low))
            else:
                half_tile = jnp.where(left, turned(top), low)
            sends[cls][n, :odd] = half_tile.astype(jnp.bfloat16)
            for i in range(full):
                here = slice(odd + i * TILE, odd + (i + 1) * TILE)
                sends[cls][n, here] = tile(whole[n] + i).astype(jnp.bfloat16)
        if cls == 2:
            wd[f] = sends[cls][q]
        else:
            slot[cls][f, TILE:] = sends[cls][q]

    def unfold(i):
        for where in (wg, wu):
            folded = where[i, TILE : TILE + odd].astype(jnp.float32)
            where[i, :odd] = jnp.where(left, folded, 0.0).astype(jnp.bfloat16)
            where[i, odd:TILE] = jnp.where(left, turned(folded), 0.0).astype(jnp.bfloat16)

    def cut(cls, i):
        return wd.at[i] if cls == 2 else slot[cls].at[i, pl.ds(TILE, part)]

    def rsh(cls, k):
        return rcopy(
            sends[cls].at[qk[k]], cut(cls, f),
            rsh_send.at[cls, k - 1], rsh_recv.at[cls, k - 1], at(k),
        )

    def rsh_start(cls, k):
        rsh(cls, k).start()

    def rsh_wait(cls, k):
        where = cut(cls, 4 * z + qk[k])
        rcopy(where, where, rsh_send.at[cls, k - 1], rsh_recv.at[cls, k - 1], at(k)).wait_recv()

    def zcopy(cls, i, d):
        dev = (f + 4, c) if d == 0 else (f - 4, c)
        return rcopy(cut(cls, i), cut(cls, i), z_send.at[d, cls, i], z_recv.at[cls, i], dev)

    def inward(cls, i):
        pl.when(z < 2)(lambda: zcopy(cls, i, 0).start())
        pl.when(z > 1)(lambda: zcopy(cls, i, 1).start())

    def outward(cls, i):
        pl.when(z == 2)(lambda: zcopy(cls, i, 0).start())
        pl.when(z == 1)(lambda: zcopy(cls, i, 1).start())

    inner, outer = (z == 1) | (z == 2), (z == 0) | (z == 3)

    def relay(cls, r, ks, who=None):
        who = z >= 0 if who is None else who
        for k in ks:
            j = qk[k] if cls < 2 else k
            low, high = 4 * (z - r) + j, 4 * (z + r) + j

            @pl.when(who & (z >= r))
            def _():
                zcopy(cls, low, 0).wait_recv()
                if r < 3:
                    pl.when(z < 3)(lambda: zcopy(cls, low, 0).start())

            @pl.when(who & (z + r <= 3))
            def _():
                zcopy(cls, high, 1).wait_recv()
                if r < 3:
                    pl.when(z > 0)(lambda: zcopy(cls, high, 1).start())

    for copy in loads[0]:
        copy.wait()
    rounded(0)
    pl.semaphore_wait(barrier, 4 + jnp.minimum(z, 1) + jnp.minimum(3 - z, 1))
    outward(0, f)
    inward(0, f)
    for k in (1, 2, 3):
        rsh_start(0, k)
    for copy in loads[1]:
        copy.wait()
    rounded(1)
    outward(1, f)
    inward(1, f)
    for k in (1, 2, 3):
        rsh_start(1, k)
    load_d.wait()
    rounded(2)
    for k in (1, 2, 3):
        rsh_start(2, k)
    def both(r, ks):
        for k in ks:
            relay(0, r, (k,))
            relay(1, r, (k,))

    def piece(core, h):
        return pl.ds(pl.multiple_of(half * core + h * quarter, 16), quarter)

    def xcopy(owner, h, ssem, rsem, dev):
        where = xbuf.at[qk[owner], piece(c, h), :]
        return rcopy(where, where, ssem, rsem, dev)

    def direct(k, h, owner):
        return xcopy(owner, h, x_send.at[k - 1, h], x_recv.at[k - 1, h], at(k))

    def onward(h, owner):
        return xcopy(owner, h, x_send.at[2, h], x_recv.at[2, h], at(2 if h == 0 else 1))

    def share(k, h, core):
        where = xbuf.at[qk[k], piece(core, h), :]
        return rcopy(where, where, s_send.at[k, h], s_recv.at[k, h], partner)

    def own_plane(cls):
        for k in (1, 2, 3):
            rsh_wait(cls, k)
            outward(cls, 4 * z + qk[k])
            inward(cls, 4 * z + qk[k])

    own_plane(0)
    load_x.wait()

    def normalize(m, _):
        here = pl.ds(pl.multiple_of(half * c + m * 16, 16), 16)
        values = xbuf[q, here, :].astype(jnp.float32)
        scale = lax.rsqrt(jnp.mean(values * values, axis=-1, keepdims=True) + 1e-06)
        xbuf[q, here, :] = (values * scale * ng_ref[...]).astype(jnp.bfloat16)
        return 0

    lax.fori_loop(0, half // 16, normalize, 0)

    direct(1, 0, 0).start()
    direct(2, 1, 0).start()
    direct(1, 1, 0).start()
    direct(2, 0, 0).start()
    for h in (0, 1):
        share(0, h, c).start()
    own_plane(1)

    side = lax.div(z, 2)
    zz = z + side * (3 - 2 * z)

    def turn(t):
        base = t if t >= 2 else lax.rem(t + zz, 2)
        return base + side * (3 - 2 * base)

    def columns(s, h=None):
        if h is None:
            return pl.ds(pl.multiple_of(s * width, TILE), width)
        return pl.ds(pl.multiple_of(s * width + h * pair, TILE), pair)

    def gate_up(t, k0, k1, portion=None, fresh=True):
        s = turn(t)
        if portion is None:
            blocks, across = [4 * s + i for i in range(4)], columns(s)
        else:
            side = lax.rem(lax.div(q, 2) + portion, 2)
            blocks, across = [4 * s + 2 * side + i for i in (0, 1)], columns(s, side)

        if fresh:
            for i in blocks:
                unfold(i)

        def step(m, _):
            who = chip(lax.div(m, hi // 2))
            n = lax.rem(m, hi // 2)
            here = pl.ds(pl.multiple_of(who * rows, 16), rows)
            cols = pl.ds(pl.multiple_of(n * pair, TILE), pair)
            one = pl.ds(pl.multiple_of(n * pair + odd * jnp.minimum(n, 1), odd), TILE)
            two = pl.ds(pl.multiple_of(n * pair + TILE + odd, odd), TILE)
            found = []
            for j, acc in enumerate((accg, accu)):
                w = jnp.concatenate([
                    jnp.concatenate([slot[j][i, one, :], slot[j][i, two, :]], axis=1) for i in blocks
                ], axis=0)
                x = xbuf[who, :, across]
                part_sum = lax.dot_general(x, w, NN, preferred_element_type=jnp.float32)
                if t > 0:
                    part_sum = part_sum + acc[here, cols]
                if portion != 1:
                    acc[here, cols] = part_sum
                found.append(part_sum)
            if portion == 1:
                g = found[0] * scl[0:1, cols]
                u = found[1] * scl[1:2, cols]
                hid[here, cols] = (g / (1.0 + jnp.exp(-g)) * u).astype(jnp.bfloat16)
            return 0

        lax.fori_loop(k0 * (hi // 2), k1 * (hi // 2), step, 0)

    both(1, range(4))
    for h in (0, 1):
        share(0, h, 1 - c).wait_recv()
    direct(1, 0, 1).wait_recv()
    onward(0, 1).start()
    share(1, 0, c).start()
    direct(2, 1, 2).wait_recv()
    onward(1, 2).start()
    share(2, 1, c).start()
    for k in (1, 2, 3):
        rsh_wait(2, k)
    for j in range(4):
        inward(2, 4 * z + j)
    both(2, range(3))
    direct(1, 1, 1).wait_recv()
    share(1, 1, c).start()
    direct(2, 0, 2).wait_recv()
    share(2, 0, c).start()
    for k in (1, 2):
        for h in (0, 1):
            share(k, h, 1 - c).wait_recv()
    gate_up(0, 0, 3)
    both(2, (3,))
    for j in range(4):
        outward(2, 4 * z + j)
    gate_up(1, 0, 3)
    gate_up(2, 0, 3)
    onward(0, 3).wait_recv()
    share(3, 0, c).start()
    onward(1, 3).wait_recv()
    share(3, 1, c).start()
    for h in (0, 1):
        share(3, h, 1 - c).wait_recv()
    for t in range(3):
        gate_up(t, 3, 4, None, False)
    for h in (0, 1):
        direct(1, h, 0).wait_send()
        direct(2, h, 0).wait_send()
        onward(h, 1 + h).wait_send()
        for k in range(4):
            share(k, h, c).wait_send()
    def spot(u):
        s = turn(u // 2)
        return 2 * lax.rem(s, 2) + u % 2, columns(s, u % 2), lax.div(s, 2)

    def pcopy(i, cols, k):
        return rcopy(
            xbuf.at[chip(k), :, cols], pbuf.at[i, k], p_send.at[i, k], p_recv.at[i, k], partner
        )

    def product(u, k):
        i, cols, owner = spot(u)
        block = 4 * turn(u // 2) + 2 * (u % 2)
        here = pl.ds(pl.multiple_of(chip(k) * rows, 16), rows)
        nothing = jnp.zeros((TILE - odd, TILE), jnp.bfloat16)
        w = jnp.concatenate([
            jnp.concatenate([wd[block + n, :odd], nothing, wd[block + n, odd:]], axis=0) for n in (0, 1)
        ], axis=1)
        o = lax.dot_general(hid[here, :], w, NN, preferred_element_type=jnp.float32)
        xbuf[chip(k), :, cols] = o.astype(jnp.bfloat16)
        pl.when(owner != c)(lambda: pcopy(i, cols, k).start())

    def products(u):
        def step(n, _):
            product(u, 3 - n)
            return 0

        lax.fori_loop(0, 4, step, 0)

    places = ((1, 0, 1), (3, 0, 1), (2, 1, 2), (3, 1, 2), (2, 0, 2), (1, 1, 1))

    def scopy(i, cols, place):
        k, h, to = places[place]
        return rcopy(
            xbuf.at[qk[k], pl.ds(h * half, half), cols], rbuf.at[i, place],
            r_send.at[i, place], r_recv.at[i, place], at(to),
        )

    def added(k, first_row, n_rows, cols, more):
        who = chip(k)

        def step(m, _):
            here = pl.ds(pl.multiple_of(first_row + m * TILE, 16), TILE)
            there = pl.ds(pl.multiple_of(m * TILE, 16), TILE)
            both = xbuf[who, here, cols].astype(jnp.float32) + more[there, :].astype(jnp.float32)
            xbuf[who, here, cols] = both.astype(jnp.bfloat16)
            return 0

        lax.fori_loop(0, n_rows // TILE, step, 0)

    def finish(u, k):
        i, cols, owner = spot(u)

        @pl.when(owner == c)
        def _():
            pcopy(i, cols, k).wait_recv()
            added(k, 0, rows, cols, pbuf.at[i, k])

            @pl.when(k == 3)
            def _():
                scopy(i, cols, 1).start()
                scopy(i, cols, 3).start()

            pl.when(k == 2)(lambda: scopy(i, cols, 2).start())
            pl.when(k == 1)(lambda: scopy(i, cols, 0).start())

    def finish_all(u):
        def step(n, _):
            finish(u, 3 - n)
            return 0

        lax.fori_loop(0, 4, step, 0)

    def second(u):
        i, cols, owner = spot(u)

        @pl.when(owner == c)
        def _():
            for came, goes in ((1, 4), (3, 5)):
                scopy(i, cols, came).wait_recv()
                k, h, _ = places[goes]
                added(k, h * half, half, cols, rbuf.at[i, came])
                scopy(i, cols, goes).start()

    def final(u):
        i, cols, owner = spot(u)

        @pl.when(owner == c)
        def _():
            there = pl.ds(pl.multiple_of(i * pair, TILE), pair)
            for h, (one, two) in enumerate(((0, 4), (2, 5))):
                scopy(i, cols, one).wait_recv()
                scopy(i, cols, two).wait_recv()

                def step(m, _):
                    here = pl.ds(pl.multiple_of(h * half + m * TILE, 16), TILE)
                    part = pl.ds(pl.multiple_of(m * TILE, 16), TILE)
                    total = (
                        xbuf[q, here, cols].astype(jnp.float32)
                        + rbuf[i, one, part, :].astype(jnp.float32)
                        + rbuf[i, two, part, :].astype(jnp.float32)
                    )
                    out_ref[here, there] = (total * ds_ref[:, there]).astype(jnp.bfloat16)
                    return 0

                lax.fori_loop(0, half // TILE, step, 0)

    both(3, (0, 1))
    gate_up(3, 0, 4, 0)
    both(3, (2, 3))
    for i in (0, 1):
        unfold(4 * turn(3) + 2 * lax.rem(lax.div(q, 2) + 1, 2) + i)

    def begin(n, _):
        gate_up(3, 3 - n, 4 - n, 1, False)
        product(0, 3 - n)
        pl.when(n > 0)(lambda: finish(0, 4 - n))
        return 0

    lax.fori_loop(0, 4, begin, 0)
    finish(0, 0)
    products(1)
    finish_all(1)
    second(0)
    for u in range(2, 7):
        relay(2, u // 2, (2 * (u % 2), 2 * (u % 2) + 1))
        products(u)
        finish_all(u)
        second(u - 1)
        if u > 3:
            final(u - 4)
    relay(2, 3, (2, 3))
    products(7)
    finish_all(7)
    second(6)
    for u in range(3, 6):
        final(u)
    second(7)
    final(6)
    final(7)

    for cls in (0, 1, 2):
        for k in (1, 2, 3):
            rsh(cls, k).wait_send()
        for r in range(3):
            for k in range(4):
                low, high = 4 * (z - r) + qk[k], 4 * (z + r) + qk[k]
                pl.when((z >= r) & (z < 3))(
                    lambda: zcopy(cls, low, 0).wait_send()
                )
                pl.when((z + r <= 3) & (z > 0))(
                    lambda: zcopy(cls, high, 1).wait_send()
                )
    for u in range(8):
        i, cols, owner = spot(u)

        @pl.when(owner == c)
        def _():
            for place in range(6):
                scopy(i, cols, place).wait_send()

        @pl.when(owner != c)
        def _():
            for k in range(4):
                pcopy(i, cols, k).wait_send()


def planes(tokens, norm_gain, gate_weight, up_weight, gate_scale, up_scale, down_weight, down_scale):
    rows, model = tokens.shape
    units = gate_weight.shape[1]
    tiles, part = units // TILE, units // 4
    hi = -(-part // TILE)
    bf, f32, dma = jnp.bfloat16, jnp.float32, pltpu.SemaphoreType.DMA
    hbm = pl.BlockSpec(memory_space=pl.ANY)
    vmem = pl.BlockSpec(memory_space=pltpu.VMEM)
    return pl.pallas_call(
        kernel,
        out_shape=jax.ShapeDtypeStruct((rows, down_scale.shape[0]), bf),
        in_specs=[hbm, hbm, hbm, hbm, vmem, vmem, vmem, vmem],
        out_specs=vmem,
        scratch_shapes=[
            pltpu.VMEM((4, rows, model), bf),
            pltpu.VMEM((16, TILE + part, TILE), bf),
            pltpu.VMEM((16, TILE + part, TILE), bf),
            pltpu.VMEM((16, part, TILE), bf),
            pltpu.VMEM((4, part, TILE), bf),
            pltpu.VMEM((4, part, TILE), bf),
            pltpu.VMEM((4, part, TILE), bf),
            pltpu.VMEM((4 * rows, hi * TILE), f32),
            pltpu.VMEM((4 * rows, hi * TILE), f32),
            pltpu.VMEM((4 * rows, hi * TILE), bf),
            pltpu.VMEM((4, 4, rows, 2 * TILE), bf),
            pltpu.VMEM((4, 6, rows // 2, 2 * TILE), bf),
            pltpu.VMEM((8, hi * TILE), f32),
            dma((3, 4)), dma((3, 3)), dma((3, 3)),
            dma((3, 2)), dma((3, 2)), dma((4, 2)), dma((4, 2)),
            dma((2, 3, 16)), dma((3, 16)),
            dma((4, 4)), dma((4, 4)), dma((4, 6)), dma((4, 6)),
        ],
        compiler_params=pltpu.CompilerParams(
            collective_id=0, has_side_effects=True, vmem_limit_bytes=67043328
        ),
    )(
        gate_weight, up_weight, down_weight, tokens,
        norm_gain[None], gate_scale.reshape(tiles, TILE), up_scale.reshape(tiles, TILE), down_scale[None],
    )


def solution(mesh):
    in_specs = (
        P("fs", None),
        P(),
        P("fs", "tp"),
        P("fs", "tp"),
        P("tp"),
        P("tp"),
        P("tp", "fs"),
        P("tp"),
    )
    out_specs = P("fs", "tp")
    body = planes if (mesh.shape["fs"], mesh.shape["tp"]) == (16, 2) else gathered
    return jax.shard_map(body, mesh=mesh, in_specs=in_specs, out_specs=out_specs, check_vma=False)
```

```python
import jax
import jax.numpy as jnp
from jax import lax
from jax.experimental import pallas as pl
from jax.experimental.pallas import tpu as pltpu
from jax.sharding import PartitionSpec as P

MESH = pl.DeviceIdType.MESH
NN = (((1,), (0,)), ((), ()))
TILE = 128


def norm(tokens, norm_gain):
    values = tokens.astype(jnp.float32)
    return (
        values * lax.rsqrt(jnp.mean(values * values, axis=-1, keepdims=True) + 1e-06) * norm_gain
    ).astype(jnp.bfloat16)


def gathered(tokens, norm_gain, gate_weight, up_weight, gate_scale, up_scale, down_weight, down_scale):
    normed = norm(tokens, norm_gain)

    def add_rows(piece):
        return jnp.dot(normed, piece, preferred_element_type=jnp.float32)

    gate = add_rows(lax.all_gather(gate_weight.astype(jnp.bfloat16), "fs", axis=0, tiled=True))
    up = add_rows(lax.all_gather(up_weight.astype(jnp.bfloat16), "fs", axis=0, tiled=True))
    hidden = (jax.nn.silu(gate * gate_scale) * (up * up_scale)).astype(jnp.bfloat16)
    terms = jnp.dot(
        hidden,
        lax.all_gather(down_weight.astype(jnp.bfloat16), "fs", axis=1, tiled=True),
        preferred_element_type=jnp.float32,
    )
    summed = lax.psum_scatter(
        terms.astype(jnp.bfloat16), "tp", scatter_dimension=1, tiled=True
    ).astype(jnp.float32)
    return (summed * down_scale).astype(jnp.bfloat16)


def kernel(
    g_ref, u_ref, d_ref, x_ref, ng_ref, gs_ref, us_ref, ds_ref, out_ref,
    xbuf, wg, wu, wd, gsend, usend, dsend, accg, accu, hid, pbuf, rbuf, scl,
    l_sem, rsh_send, rsh_recv, x_send, x_recv, s_send, s_recv,
    z_send, z_recv, p_send, p_recv, r_send, r_recv,
):
    f, c = lax.axis_index("fs"), lax.axis_index("tp")
    z, q = lax.div(f, 4), lax.rem(f, 4)
    qk = [q, q + 1 - 2 * lax.rem(q, 2), lax.rem(q + 2, 4), 3 - q]
    slot, sends = (wg, wu, wd), (gsend, usend, dsend)
    part = wd.shape[1]
    tiles, full, odd = 4 * part // TILE, part // TILE, part % TILE
    hi = full + 1
    rows = x_ref.shape[0]
    half, quarter = rows // 2, rows // 4
    width = 4 * TILE
    pair = 2 * TILE
    partner = (f, 1 - c)

    def at(k):
        return (4 * z + qk[k], c)

    def chip(k):
        return lax.rem(q + k, 2) + 2 * lax.rem(lax.div(q, 2) + lax.div(k, 2), 2)

    def rcopy(src, dst, ssem, rsem, dev):
        return pltpu.make_async_remote_copy(
            src_ref=src, dst_ref=dst, send_sem=ssem, recv_sem=rsem,
            device_id=dev, device_id_type=MESH,
        )

    barrier = pltpu.get_barrier_semaphore()

    def greet(dev):
        pl.semaphore_signal(barrier, inc=1, device_id=dev, device_id_type=MESH)

    greet(partner)
    for k in (1, 2, 3):
        greet(at(k))
    pl.when(z > 0)(lambda: greet((f - 4, c)))
    pl.when(z < 3)(lambda: greet((f + 4, c)))

    slab = hi * TILE
    cuts = [(i, min(slab, tiles * TILE - i)) for i in range(0, tiles * TILE, slab)]
    loads = ([], [])
    for j, ref in enumerate((g_ref, u_ref)):
        for n, (i, w) in enumerate(cuts):
            loads[j].append(pltpu.make_async_copy(
                ref.at[:, pl.ds(i, w)],
                accg.at[pl.ds((j * len(cuts) + n) * TILE, TILE), pl.ds(0, w)],
                l_sem.at[j, n],
            ))
    load_d = pltpu.make_async_copy(
        d_ref, accu.at[pl.ds(0, tiles * TILE), pl.ds(0, TILE)], l_sem.at[2, 0]
    )
    mine = pl.ds(pl.multiple_of(half * c, 16), half)
    load_x = pltpu.make_async_copy(x_ref.at[mine, :], xbuf.at[q, mine, :], l_sem.at[2, 1])
    for copy in loads[0]:
        copy.start()

    def turned(value):
        return pltpu.roll(value, odd, 1)

    left = lax.broadcasted_iota(jnp.int32, (odd, TILE), 1) < odd
    whole = [full * n + (n + 1) // 2 for n in range(4)]
    split = [full + (full + hi) * (n // 2) for n in range(4)]
    for j, ref in enumerate((gs_ref, us_ref)):
        row = jnp.broadcast_to(ref[pl.ds(full + (full + hi) * lax.div(q, 2), 1), :], (8, TILE))
        row = jnp.where(lax.rem(q, 2) == 0, row, turned(row))
        scl[j : j + 1, :TILE] = row[0:1]
        for i in range(full):
            at_tile = full * q + lax.div(q + 1, 2) + i
            scl[j : j + 1, (i + 1) * TILE : (i + 2) * TILE] = ref[pl.ds(at_tile, 1), :]

    for copy in loads[1]:
        copy.start()
    load_d.start()
    load_x.start()

    def rounded(cls):
        def tile(i):
            if cls == 2:
                return accu[i * TILE : (i + 1) * TILE, :TILE]
            top = (cls * len(cuts) + i // hi) * TILE
            return accg[top : top + TILE, i % hi * TILE : (i % hi + 1) * TILE]

        for n in range(4):
            both = tile(split[n])
            top, low = both[:odd], both[odd:]
            if cls == 2:
                half_tile = top if n % 2 == 0 else low
            elif n % 2 == 0:
                half_tile = jnp.where(left, top, turned(low))
            else:
                half_tile = jnp.where(left, turned(top), low)
            sends[cls][n, :odd] = half_tile.astype(jnp.bfloat16)
            for i in range(full):
                here = slice(odd + i * TILE, odd + (i + 1) * TILE)
                sends[cls][n, here] = tile(whole[n] + i).astype(jnp.bfloat16)
        if cls == 2:
            wd[f] = sends[cls][q]
        else:
            slot[cls][f, TILE:] = sends[cls][q]

    def unfold(i):
        for where in (wg, wu):
            folded = where[i, TILE : TILE + odd].astype(jnp.float32)
            where[i, :odd] = jnp.where(left, folded, 0.0).astype(jnp.bfloat16)
            where[i, odd:TILE] = jnp.where(left, turned(folded), 0.0).astype(jnp.bfloat16)

    def cut(cls, i):
        return wd.at[i] if cls == 2 else slot[cls].at[i, pl.ds(TILE, part)]

    def rsh(cls, k):
        return rcopy(
            sends[cls].at[qk[k]], cut(cls, f),
            rsh_send.at[cls, k - 1], rsh_recv.at[cls, k - 1], at(k),
        )

    def rsh_start(cls, k):
        rsh(cls, k).start()

    def rsh_wait(cls, k):
        where = cut(cls, 4 * z + qk[k])
        rcopy(where, where, rsh_send.at[cls, k - 1], rsh_recv.at[cls, k - 1], at(k)).wait_recv()

    def zcopy(cls, i, d):
        dev = (f + 4, c) if d == 0 else (f - 4, c)
        return rcopy(cut(cls, i), cut(cls, i), z_send.at[d, cls, i], z_recv.at[cls, i], dev)

    def inward(cls, i):
        pl.when(z < 2)(lambda: zcopy(cls, i, 0).start())
        pl.when(z > 1)(lambda: zcopy(cls, i, 1).start())

    def outward(cls, i):
        pl.when(z == 2)(lambda: zcopy(cls, i, 0).start())
        pl.when(z == 1)(lambda: zcopy(cls, i, 1).start())

    inner, outer = (z == 1) | (z == 2), (z == 0) | (z == 3)

    def relay(cls, r, ks, who=None):
        who = z >= 0 if who is None else who
        for k in ks:
            j = qk[k] if cls < 2 else k
            low, high = 4 * (z - r) + j, 4 * (z + r) + j

            @pl.when(who & (z >= r))
            def _():
                zcopy(cls, low, 0).wait_recv()
                if r < 3:
                    pl.when(z < 3)(lambda: zcopy(cls, low, 0).start())

            @pl.when(who & (z + r <= 3))
            def _():
                zcopy(cls, high, 1).wait_recv()
                if r < 3:
                    pl.when(z > 0)(lambda: zcopy(cls, high, 1).start())

    for copy in loads[0]:
        copy.wait()
    rounded(0)
    pl.semaphore_wait(barrier, 4 + jnp.minimum(z, 1) + jnp.minimum(3 - z, 1))
    outward(0, f)
    inward(0, f)
    for k in (1, 2, 3):
        rsh_start(0, k)
    for copy in loads[1]:
        copy.wait()
    rounded(1)
    outward(1, f)
    inward(1, f)
    for k in (1, 2, 3):
        rsh_start(1, k)
    load_d.wait()
    rounded(2)
    for k in (1, 2, 3):
        rsh_start(2, k)
    def both(r, ks):
        for k in ks:
            relay(0, r, (k,))
            relay(1, r, (k,))

    def piece(core, h):
        return pl.ds(pl.multiple_of(half * core + h * quarter, 16), quarter)

    def xcopy(owner, h, ssem, rsem, dev):
        where = xbuf.at[qk[owner], piece(c, h), :]
        return rcopy(where, where, ssem, rsem, dev)

    def direct(k, h, owner):
        return xcopy(owner, h, x_send.at[k - 1, h], x_recv.at[k - 1, h], at(k))

    def onward(h, owner):
        return xcopy(owner, h, x_send.at[2, h], x_recv.at[2, h], at(2 if h == 0 else 1))

    def share(k, h, core):
        where = xbuf.at[qk[k], piece(core, h), :]
        return rcopy(where, where, s_send.at[k, h], s_recv.at[k, h], partner)

    def own_plane(cls):
        for k in (1, 2, 3):
            rsh_wait(cls, k)
            outward(cls, 4 * z + qk[k])
            inward(cls, 4 * z + qk[k])

    own_plane(0)
    load_x.wait()

    def normalize(m, _):
        here = pl.ds(pl.multiple_of(half * c + m * 16, 16), 16)
        values = xbuf[q, here, :].astype(jnp.float32)
        scale = lax.rsqrt(jnp.mean(values * values, axis=-1, keepdims=True) + 1e-06)
        xbuf[q, here, :] = (values * scale * ng_ref[...]).astype(jnp.bfloat16)
        return 0

    lax.fori_loop(0, half // 16, normalize, 0)

    direct(1, 0, 0).start()
    direct(2, 1, 0).start()
    direct(1, 1, 0).start()
    direct(2, 0, 0).start()
    for h in (0, 1):
        share(0, h, c).start()
    own_plane(1)

    side = lax.div(z, 2)
    zz = z + side * (3 - 2 * z)

    def turn(t):
        base = t if t >= 2 else lax.rem(t + zz, 2)
        return base + side * (3 - 2 * base)

    def columns(s, h=None):
        if h is None:
            return pl.ds(pl.multiple_of(s * width, TILE), width)
        return pl.ds(pl.multiple_of(s * width + h * pair, TILE), pair)

    def gate_up(t, k0, k1, portion=None, fresh=True):
        s = turn(t)
        if portion is None:
            blocks, across = [4 * s + i for i in range(4)], columns(s)
        else:
            side = lax.rem(lax.div(q, 2) + portion, 2)
            blocks, across = [4 * s + 2 * side + i for i in (0, 1)], columns(s, side)

        if fresh:
            for i in blocks:
                unfold(i)

        def step(m, _):
            who = chip(lax.div(m, hi // 2))
            n = lax.rem(m, hi // 2)
            here = pl.ds(pl.multiple_of(who * rows, 16), rows)
            cols = pl.ds(pl.multiple_of(n * pair, TILE), pair)
            one = pl.ds(pl.multiple_of(n * pair + odd * jnp.minimum(n, 1), odd), TILE)
            two = pl.ds(pl.multiple_of(n * pair + TILE + odd, odd), TILE)
            found = []
            for j, acc in enumerate((accg, accu)):
                w = jnp.concatenate([
                    jnp.concatenate([slot[j][i, one, :], slot[j][i, two, :]], axis=1) for i in blocks
                ], axis=0)
                x = xbuf[who, :, across]
                part_sum = lax.dot_general(x, w, NN, preferred_element_type=jnp.float32)
                if t > 0:
                    part_sum = part_sum + acc[here, cols]
                if portion != 1:
                    acc[here, cols] = part_sum
                found.append(part_sum)
            if portion == 1:
                g = found[0] * scl[0:1, cols]
                u = found[1] * scl[1:2, cols]
                hid[here, cols] = (g / (1.0 + jnp.exp(-g)) * u).astype(jnp.bfloat16)
            return 0

        lax.fori_loop(k0 * (hi // 2), k1 * (hi // 2), step, 0)

    both(1, range(4))
    for h in (0, 1):
        share(0, h, 1 - c).wait_recv()
    direct(1, 0, 1).wait_recv()
    onward(0, 1).start()
    share(1, 0, c).start()
    direct(2, 1, 2).wait_recv()
    onward(1, 2).start()
    share(2, 1, c).start()
    for k in (1, 2, 3):
        rsh_wait(2, k)
    for j in range(4):
        inward(2, 4 * z + j)
    both(2, range(3))
    direct(1, 1, 1).wait_recv()
    share(1, 1, c).start()
    direct(2, 0, 2).wait_recv()
    share(2, 0, c).start()
    for k in (1, 2):
        for h in (0, 1):
            share(k, h, 1 - c).wait_recv()
    gate_up(0, 0, 3)
    both(2, (3,))
    for j in range(4):
        outward(2, 4 * z + j)
    gate_up(1, 0, 3)
    gate_up(2, 0, 3)
    onward(0, 3).wait_recv()
    share(3, 0, c).start()
    onward(1, 3).wait_recv()
    share(3, 1, c).start()
    for h in (0, 1):
        share(3, h, 1 - c).wait_recv()
    for t in range(3):
        gate_up(t, 3, 4, None, False)
    for h in (0, 1):
        direct(1, h, 0).wait_send()
        direct(2, h, 0).wait_send()
        onward(h, 1 + h).wait_send()
        for k in range(4):
            share(k, h, c).wait_send()
    def spot(u):
        s = turn(u // 2)
        return 2 * lax.rem(s, 2) + u % 2, columns(s, u % 2), lax.div(s, 2)

    def pcopy(i, cols, k):
        return rcopy(
            xbuf.at[chip(k), :, cols], pbuf.at[i, k], p_send.at[i, k], p_recv.at[i, k], partner
        )

    def product(u, k):
        i, cols, owner = spot(u)
        block = 4 * turn(u // 2) + 2 * (u % 2)
        here = pl.ds(pl.multiple_of(chip(k) * rows, 16), rows)
        nothing = jnp.zeros((TILE - odd, TILE), jnp.bfloat16)
        w = jnp.concatenate([
            jnp.concatenate([wd[block + n, :odd], nothing, wd[block + n, odd:]], axis=0) for n in (0, 1)
        ], axis=1)
        o = lax.dot_general(hid[here, :], w, NN, preferred_element_type=jnp.float32)
        xbuf[chip(k), :, cols] = o.astype(jnp.bfloat16)
        pl.when(owner != c)(lambda: pcopy(i, cols, k).start())

    def products(u):
        def step(n, _):
            product(u, 3 - n)
            return 0

        lax.fori_loop(0, 4, step, 0)

    places = ((1, 0, 1), (3, 0, 1), (2, 1, 2), (3, 1, 2), (2, 0, 2), (1, 1, 1))

    def scopy(i, cols, place):
        k, h, to = places[place]
        return rcopy(
            xbuf.at[qk[k], pl.ds(h * half, half), cols], rbuf.at[i, place],
            r_send.at[i, place], r_recv.at[i, place], at(to),
        )

    def added(k, first_row, n_rows, cols, more):
        who = chip(k)

        def step(m, _):
            here = pl.ds(pl.multiple_of(first_row + m * TILE, 16), TILE)
            there = pl.ds(pl.multiple_of(m * TILE, 16), TILE)
            both = xbuf[who, here, cols].astype(jnp.float32) + more[there, :].astype(jnp.float32)
            xbuf[who, here, cols] = both.astype(jnp.bfloat16)
            return 0

        lax.fori_loop(0, n_rows // TILE, step, 0)

    def finish(u, k):
        i, cols, owner = spot(u)

        @pl.when(owner == c)
        def _():
            pcopy(i, cols, k).wait_recv()
            added(k, 0, rows, cols, pbuf.at[i, k])

            @pl.when(k == 3)
            def _():
                scopy(i, cols, 1).start()
                scopy(i, cols, 3).start()

            pl.when(k == 2)(lambda: scopy(i, cols, 2).start())
            pl.when(k == 1)(lambda: scopy(i, cols, 0).start())

    def finish_all(u):
        def step(n, _):
            finish(u, 3 - n)
            return 0

        lax.fori_loop(0, 4, step, 0)

    def second(u):
        i, cols, owner = spot(u)

        @pl.when(owner == c)
        def _():
            for came, goes in ((1, 4), (3, 5)):
                scopy(i, cols, came).wait_recv()
                k, h, _ = places[goes]
                added(k, h * half, half, cols, rbuf.at[i, came])
                scopy(i, cols, goes).start()

    def result(i, cols):
        there = pl.ds(pl.multiple_of(i * pair, TILE), pair)
        return pltpu.make_async_copy(xbuf.at[q, :, cols], out_ref.at[:, there], l_sem.at[0, i])

    def final(u):
        i, cols, owner = spot(u)

        @pl.when(owner == c)
        def _():
            there = pl.ds(pl.multiple_of(i * pair, TILE), pair)
            for h, (one, two) in enumerate(((0, 4), (2, 5))):
                scopy(i, cols, one).wait_recv()
                scopy(i, cols, two).wait_recv()

                def step(m, _):
                    here = pl.ds(pl.multiple_of(h * half + m * TILE, 16), TILE)
                    part = pl.ds(pl.multiple_of(m * TILE, 16), TILE)
                    total = (
                        xbuf[q, here, cols].astype(jnp.float32)
                        + rbuf[i, one, part, :].astype(jnp.float32)
                        + rbuf[i, two, part, :].astype(jnp.float32)
                    )
                    xbuf[q, here, cols] = (total * ds_ref[:, there]).astype(jnp.bfloat16)
                    return 0

                lax.fori_loop(0, half // TILE, step, 0)
            result(i, cols).start()

    both(3, (0, 1))
    gate_up(3, 0, 4, 0)
    both(3, (2, 3))
    for i in (0, 1):
        unfold(4 * turn(3) + 2 * lax.rem(lax.div(q, 2) + 1, 2) + i)

    def begin(n, _):
        gate_up(3, 3 - n, 4 - n, 1, False)
        product(0, 3 - n)
        pl.when(n > 0)(lambda: finish(0, 4 - n))
        return 0

    lax.fori_loop(0, 4, begin, 0)
    finish(0, 0)
    products(1)
    finish_all(1)
    second(0)
    for u in range(2, 7):
        relay(2, u // 2, (2 * (u % 2), 2 * (u % 2) + 1))
        products(u)
        finish_all(u)
        second(u - 1)
        if u > 3:
            final(u - 4)
    relay(2, 3, (2, 3))
    products(7)
    finish_all(7)
    second(6)
    for u in range(3, 6):
        final(u)
    second(7)
    final(6)
    final(7)

    for cls in (0, 1, 2):
        for k in (1, 2, 3):
            rsh(cls, k).wait_send()
        for r in range(3):
            for k in range(4):
                low, high = 4 * (z - r) + qk[k], 4 * (z + r) + qk[k]
                pl.when((z >= r) & (z < 3))(
                    lambda: zcopy(cls, low, 0).wait_send()
                )
                pl.when((z + r <= 3) & (z > 0))(
                    lambda: zcopy(cls, high, 1).wait_send()
                )
    for u in range(8):
        i, cols, owner = spot(u)

        @pl.when(owner == c)
        def _():
            result(i, cols).wait()
            for place in range(6):
                scopy(i, cols, place).wait_send()

        @pl.when(owner != c)
        def _():
            for k in range(4):
                pcopy(i, cols, k).wait_send()


def handed_on(in_ref, out_ref, held, in_sem, out_sem):
    pieces = in_sem.shape[0]
    rows = held.shape[0] // pieces

    def copies(n, out):
        here = pl.ds(n * rows, rows)
        if out:
            return pltpu.make_async_copy(held.at[here, :], out_ref.at[here, :], out_sem.at[n])
        return pltpu.make_async_copy(in_ref.at[here, :], held.at[here, :], in_sem.at[n])

    for n in range(pieces):
        copies(n, False).start()
    for n in range(pieces):
        copies(n, False).wait()
        copies(n, True).start()
    for n in range(pieces):
        copies(n, True).wait()


def planes(tokens, norm_gain, gate_weight, up_weight, gate_scale, up_scale, down_weight, down_scale):
    rows, model = tokens.shape
    units = gate_weight.shape[1]
    tiles, part = units // TILE, units // 4
    hi = -(-part // TILE)
    bf, f32, dma = jnp.bfloat16, jnp.float32, pltpu.SemaphoreType.DMA
    hbm = pl.BlockSpec(memory_space=pl.ANY)
    vmem = pl.BlockSpec(memory_space=pltpu.VMEM)
    summed = pl.pallas_call(
        kernel,
        out_shape=jax.ShapeDtypeStruct((rows, down_scale.shape[0]), bf),
        in_specs=[hbm, hbm, hbm, hbm, vmem, vmem, vmem, vmem],
        out_specs=hbm,
        scratch_shapes=[
            pltpu.VMEM((4, rows, model), bf),
            pltpu.VMEM((16, TILE + part, TILE), bf),
            pltpu.VMEM((16, TILE + part, TILE), bf),
            pltpu.VMEM((16, part, TILE), bf),
            pltpu.VMEM((4, part, TILE), bf),
            pltpu.VMEM((4, part, TILE), bf),
            pltpu.VMEM((4, part, TILE), bf),
            pltpu.VMEM((4 * rows, hi * TILE), f32),
            pltpu.VMEM((4 * rows, hi * TILE), f32),
            pltpu.VMEM((4 * rows, hi * TILE), bf),
            pltpu.VMEM((4, 4, rows, 2 * TILE), bf),
            pltpu.VMEM((4, 6, rows // 2, 2 * TILE), bf),
            pltpu.VMEM((8, hi * TILE), f32),
            dma((3, 4)), dma((3, 3)), dma((3, 3)),
            dma((3, 2)), dma((3, 2)), dma((4, 2)), dma((4, 2)),
            dma((2, 3, 16)), dma((3, 16)),
            dma((4, 4)), dma((4, 4)), dma((4, 6)), dma((4, 6)),
        ],
        compiler_params=pltpu.CompilerParams(
            collective_id=0, has_side_effects=True, vmem_limit_bytes=67043328
        ),
    )(
        gate_weight, up_weight, down_weight, tokens,
        norm_gain[None], gate_scale.reshape(tiles, TILE), up_scale.reshape(tiles, TILE), down_scale[None],
    )
    pieces = 4
    return pl.pallas_call(
        handed_on,
        out_shape=jax.ShapeDtypeStruct(summed.shape, bf),
        in_specs=[hbm],
        out_specs=hbm,
        scratch_shapes=[pltpu.VMEM(summed.shape, bf), dma((pieces,)), dma((pieces,))],
    )(summed)


def solution(mesh):
    in_specs = (
        P("fs", None),
        P(),
        P("fs", "tp"),
        P("fs", "tp"),
        P("tp"),
        P("tp"),
        P("tp", "fs"),
        P("tp"),
    )
    out_specs = P("fs", "tp")
    body = planes if (mesh.shape["fs"], mesh.shape["tp"]) == (16, 2) else gathered
    return jax.shard_map(body, mesh=mesh, in_specs=in_specs, out_specs=out_specs, check_vma=False)
```
